32 devices in a mesh: ra: 4 (over z), cb: 4 (over y, x), dp: 2 (over core).
Axes of the slice: x: 2, y: 2, z: 4, core: 2. Of those that a mesh axis runs over, the one named last changes fastest.
Arguments:
- tokens: bfloat16 [512, 4096], P('dp', 'ra'), may hold values from -6 to 6, as said below
- pre_gain_first: bfloat16 [4096], P('ra'), may hold values from 0.099609375 to 1.8984375
- gate_first: bfloat16 [4096, 11264], P('ra', 'cb'), may hold values from -0.1875 to 0.1875
- up_first: bfloat16 [4096, 11264], P('ra', 'cb'), may hold values from -0.09375 to 0.09375
- down_first: bfloat16 [11264, 4096], P('cb', 'ra'), may hold values from -1 to 1, as said below
- post_gain_first: bfloat16 [4096], P('ra'), may hold values from 0.099609375 to 1.8984375
- pre_gain_second: bfloat16 [4096], P('ra'), may hold values from 0.099609375 to 1.8984375
- gate_second: bfloat16 [4096, 11264], P('ra', 'cb'), may hold values from -0.1875 to 0.1875
- up_second: bfloat16 [4096, 11264], P('ra', 'cb'), may hold values from -0.09375 to 0.09375
- down_second: bfloat16 [11264, 4096], P('cb', 'ra'), may hold values from -1 to 1, as said below
- post_gain_second: bfloat16 [4096], P('ra'), may hold values from 0.099609375 to 1.8984375
Outputs:
- stream_out: float32 [512, 4096], P('dp', 'ra')
The draws below stay inside these ranges and needn't reach their ends.
Inputs may be any that keep to these rules, and one draw needn't show every extreme that they name: tokens: real-valued activations; groups of 256 consecutive features carry different scales, and tokens different scales. down_first: real-valued weights; groups of 256 consecutive columns carry different scales. down_second: real-valued weights; groups of 256 consecutive columns carry different scales.
All inputs are finite; a program needn't handle non-finite values.
Results may differ from the reference program's by a relative error of at most 0.034.
Values may be sent and summed in bfloat16 or wider, within the bound.
A program may use at most 128 MiB of HBM per device.

```python
import math
import jax
import jax.numpy as jnp
from jax import lax

D = 4096
FF = 11264
TOKENS = 512
N_CB = 4


def rising_scale(key, low, high):
    jitter = jnp.exp(jax.random.uniform(key, (16,), jnp.float32, -0.2, 0.2))
    ramp = jnp.exp(jnp.linspace(math.log(low), math.log(high), 16).astype(jnp.float32))
    return jnp.repeat(ramp * jitter, D // 16)


def draw_tokens(key, part):
    key_col = jax.random.fold_in(key, 11)
    key_row = jax.random.fold_in(key, 12)
    key_base = jax.random.fold_in(key, 13)
    row_scale = jnp.exp(jax.random.uniform(key_row, (TOKENS, 1), jnp.float32, math.log(0.5), math.log(2.0)))
    col_scale = rising_scale(key_col, 0.12, 1.2)
    base = jnp.clip(jax.random.normal(key_base, (TOKENS, D), jnp.float32), -4.0, 4.0)
    return (0.2 * base * row_scale * col_scale).astype(jnp.bfloat16)


def column_scaled(key, salt):
    key_col = jax.random.fold_in(key, salt)
    key_base = jax.random.fold_in(key, salt + 1)
    col_scale = rising_scale(key_col, 0.2, 2.0)
    base = jnp.clip(jax.random.normal(key_base, (FF, D), jnp.float32), -4.0, 4.0)
    return (base * col_scale * FF ** (-0.5)).astype(jnp.bfloat16)


def draw_down_first(key, part):
    return column_scaled(key, 31)


def draw_down_second(key, part):
    return column_scaled(key, 47)


def shard_levels(key, dims, cuts, low, top_value):
    level = 1.0
    for axis_at, parts in cuts:
        heights = jax.random.uniform(jax.random.fold_in(jax.random.fold_in(key, 6), axis_at), (parts,), jnp.float32, low / len(cuts), top_value / len(cuts))
        level = level * jnp.repeat(jnp.exp(heights), dims[axis_at] // parts).reshape((-1,) + (1,) * (len(dims) - 1 - axis_at))
    return level


def gaussian(own_key, extent, scale, reach, split=(), kind=jnp.bfloat16):
    values = jax.random.normal(own_key, extent, jnp.float32) * scale
    if len(split) > 0:
        values = shard_levels(own_key, extent, split, -0.22, 0.18) * values
    return jnp.clip(values, min=-reach, max=reach).astype(kind)


def setup_inputs(seed: int = 0) -> dict:
    key_list = jax.random.split(jax.random.key(seed), 12)
    return {
        "tokens": draw_tokens(jax.random.fold_in(key_list[11], 71), 0),
        "pre_gain_first": jnp.clip(1.0 + 0.18 * jax.random.normal(key_list[1], (D,), jnp.float32), 0.099609375, 1.8984375).astype(jnp.bfloat16),
        "gate_first": gaussian(key_list[2], (D, FF), (D // 4) ** -0.5, 0.1875, ((0, 4), (1, 4))),
        "up_first": gaussian(key_list[3], (D, FF), D ** -0.5, 0.09375, ((0, 4), (1, 4))),
        "down_first": draw_down_first(jax.random.fold_in(key_list[11], 71), 0),
        "post_gain_first": jnp.clip(1.0 + 0.18 * jax.random.normal(key_list[5], (D,), jnp.float32), 0.099609375, 1.8984375).astype(jnp.bfloat16),
        "pre_gain_second": jnp.clip(1.0 + 0.18 * jax.random.normal(key_list[6], (D,), jnp.float32), 0.099609375, 1.8984375).astype(jnp.bfloat16),
        "gate_second": gaussian(key_list[7], (D, FF), (D // 4) ** -0.5, 0.1875, ((0, 4), (1, 4))),
        "up_second": gaussian(key_list[8], (D, FF), D ** -0.5, 0.09375, ((0, 4), (1, 4))),
        "down_second": draw_down_second(jax.random.fold_in(key_list[11], 71), 0),
        "post_gain_second": jnp.clip(1.0 + 0.18 * jax.random.normal(key_list[10], (D,), jnp.float32), 0.099609375, 1.8984375).astype(jnp.bfloat16),
    }


EPS = 1e-06

def half_step(stream, pre_gain, gate_weight, up_weight, down_weight, post_gain):
    count = stream.shape[0]
    squares = lax.optimization_barrier(jnp.sum(stream * stream, axis=-1, keepdims=True))
    normed = (stream * lax.rsqrt(squares / D + EPS) * pre_gain.astype(jnp.float32)).astype(jnp.bfloat16)
    gate = jnp.dot(normed, gate_weight, preferred_element_type=jnp.float32)
    up = jnp.dot(normed, up_weight, preferred_element_type=jnp.float32)
    hidden = (jax.nn.silu(gate) * up).astype(jnp.bfloat16)
    groups = hidden.reshape(count, N_CB, FF // N_CB).astype(jnp.float32)
    blocks = down_weight.reshape(N_CB, FF // N_CB, D).astype(jnp.float32)
    partial_value = jnp.einsum('tgf,gfd->gtd', groups, blocks).astype(jnp.bfloat16)
    branch = lax.optimization_barrier(jnp.sum(partial_value.astype(jnp.float32), axis=0)).astype(jnp.bfloat16).astype(jnp.float32)
    branch_sq = lax.optimization_barrier(jnp.sum(branch * branch, axis=-1, keepdims=True))
    return stream + 0.5 * branch * lax.rsqrt(branch_sq / D + EPS) * post_gain.astype(jnp.float32)

def reference(tokens, pre_gain_first, gate_first, up_first, down_first, post_gain_first, pre_gain_second, gate_second, up_second, down_second, post_gain_second):
    stream = tokens.astype(jnp.float32)
    stream = half_step(stream, pre_gain_first, gate_first, up_first, down_first, post_gain_first)
    stream = half_step(stream, pre_gain_second, gate_second, up_second, down_second, post_gain_second)
    return stream
```

```python
import functools

import jax
import jax.numpy as jnp
from jax import lax
from jax.experimental import pallas as pl
from jax.experimental.pallas import tpu as pltpu
from jax.sharding import PartitionSpec as P

EPS = 1e-06
MESH = pl.DeviceIdType.MESH
F32 = jnp.float32
BF16 = jnp.bfloat16
GROUPS = 2
SLICE = 256
LAG = 2
GAP = 3 * LAG


def dot(a, b):
    return jnp.dot(a, b, preferred_element_type=F32)


def kernel(
    n_ra, tokens, g_pre0, gate0, up0, down0, g_post0, g_pre1, gate1, up1, down1, g_post1,
    out, wgu, wd, pslot, hslot, pbuf, xbuf, ybuf, acc, branch, v1, r1, v2, r2,
    stats, sst, rss, gpre, gpost,
    w_sem, p_send, p_recv, h_send, h_recv, a_send, a_recv, st_send, st_recv, ss_send, ss_recv,
):
    rows, dl = xbuf.shape
    depth = dl * n_ra
    n_k = gate0.shape[1] // SLICE
    part_rows = rows // (2 * GROUPS)
    per_layer = GROUPS * n_k
    top = n_ra - 1
    span = LAG * top
    base = n_k + 2 * span + GAP
    base = max(base, per_layer)
    half = dl // 2

    z = lax.axis_index("ra")
    c = lax.axis_index("cb")
    x_nb = c + 1 - 2 * (c % 2)
    y_nb = c + 2 - 4 * (c // 2)

    def weight_copies(i):
        layer, k = divmod(i, n_k)
        gate, up, down = ((gate0, up0, down0), (gate1, up1, down1))[layer]
        cols = pl.ds(k * SLICE, SLICE)
        return (
            pltpu.make_async_copy(gate.at[:, cols], wgu.at[i, :, pl.ds(0, SLICE)], w_sem.at[i, 0]),
            pltpu.make_async_copy(up.at[:, cols], wgu.at[i, :, pl.ds(SLICE, SLICE)], w_sem.at[i, 1]),
            pltpu.make_async_copy(down.at[cols, :], wd.at[i], w_sem.at[i, 2]),
        )

    for i in range(2 * n_k):
        for copy in weight_copies(i):
            copy.start()

    barrier = pltpu.get_barrier_semaphore()
    for j in range(1, n_ra):
        pl.semaphore_signal(barrier, inc=1, device_id={"ra": (z + j) % n_ra}, device_id_type=MESH)
    for nb in (x_nb, y_nb):
        pl.semaphore_signal(barrier, inc=1, device_id={"cb": nb}, device_id_type=MESH)
    pl.semaphore_wait(barrier, n_ra + 1)

    xbuf[...] = tokens[...].astype(F32)
    gpre[0] = g_pre0[...].astype(F32)
    gpre[1] = g_pre1[...].astype(F32)
    gpost[0] = g_post0[...].astype(F32)
    gpost[1] = g_post1[...].astype(F32)

    def item(a):
        safe = jnp.maximum(a, 0)
        layer = safe // base
        r = safe % base
        g = r // n_k
        k = r % n_k
        ok = (a >= 0) & (r < per_layer) & (layer < 2)
        return ok, layer, g, k

    def remote(src, dst, send, recv, axis, to):
        return pltpu.make_async_remote_copy(
            src_ref=src, dst_ref=dst, send_sem=send, recv_sem=recv,
            device_id={axis: to}, device_id_type=MESH,
        )

    def p_copy(s, q, to):
        return remote(pslot.at[s, q], pslot.at[s, q], p_send.at[s, q], p_recv.at[s, q], "ra", to)

    def h_copy(s, q, to):
        return remote(hslot.at[s, q], hslot.at[s, q], h_send.at[s, q], h_recv.at[s, q], "ra", to)

    def a_copy(phase, part, j):
        src, dst = ((v1, r1), (v2, r2))[phase]
        to = (x_nb, y_nb)[(phase + j) % 2]
        i = 2 * phase + j
        return remote(src.at[part, j], dst.at[part, j], a_send.at[part, i], a_recv.at[part, i], "cb", to)

    def st_copy(part, src, j):
        to = (z + j) % n_ra
        return remote(stats.at[part, src], stats.at[part, src], st_send.at[part, j], st_recv.at[part, src], "ra", to)

    def ss_copy(part, src, to):
        return remote(sst.at[part, src], sst.at[part, src], ss_send.at[part], ss_recv.at[part, src], "ra", to)

    def row_stat(sq):
        lanes = sq[:, 0:128]
        for i in range(1, dl // 128):
            lanes = lanes + sq[:, 128 * i : 128 * (i + 1)]
        got = lax.dot_general(
            jnp.ones((8, 128), F32), lanes, (((1,), (1,)), ((), ())),
            precision=lax.Precision.HIGHEST, preferred_element_type=F32,
        )
        return jnp.concatenate([got] * (128 // part_rows), axis=1)

    def scale_of(ref, part):
        total = ref[part, 0]
        for i in range(1, n_ra):
            total = total + ref[part, i]
        mean = lax.dot_general(
            total[:, 0:part_rows], jnp.full((8, 128), 0.125, F32), (((0,), (0,)), ((), ())),
            precision=lax.Precision.HIGHEST, preferred_element_type=F32,
        )
        return lax.rsqrt(mean / depth + EPS)

    def wide(scale, n):
        return jnp.concatenate([scale] * (n // 128), axis=1)

    def tick(tau, carry):
        near = jnp.minimum(z, top - z)
        ok, layer, g, k = item(tau - LAG * near)

        @pl.when(ok & (g == 0))
        def _():
            i = layer * n_k + k
            pltpu.make_async_copy(gate0.at[:, pl.ds(0, SLICE)], wgu.at[i, :, pl.ds(0, SLICE)], w_sem.at[i, 0]).wait()
            pltpu.make_async_copy(up0.at[:, pl.ds(0, SLICE)], wgu.at[i, :, pl.ds(SLICE, SLICE)], w_sem.at[i, 1]).wait()

        ok, layer, g, k = item(tau - 2 * span + LAG * (top - near))

        @pl.when(ok & (g == 0))
        def _():
            i = layer * n_k + k
            pltpu.make_async_copy(down0.at[pl.ds(0, SLICE), :], wd.at[i], w_sem.at[i, 2]).wait()

        for s in (0, 1):
            p = z if s == 0 else top - z
            onward = z + 1 if s == 0 else z - 1
            backward = z - 1 if s == 0 else z + 1
            owner = top if s == 0 else 0

            a = tau - LAG * p
            safe = jnp.maximum(a, 0)
            layer = safe // base
            r = safe % base
            g = r // n_k
            k = r % n_k
            inside = (a >= 0) & (r < per_layer)
            rs = pl.ds(pl.multiple_of((2 * g + s) * part_rows, part_rows), part_rows)

            @pl.when(inside & (k == 0) & (layer >= 1) & (layer <= 2))
            def _():
                part = ((layer - 1) * GROUPS + g) * 2 + s
                for j in range(1, n_ra):
                    st_copy(part, (z + j) % n_ra, j).wait_recv()
                scale = wide(scale_of(stats, part), dl)
                x1 = xbuf[rs, :] + 0.5 * branch[rs, :].astype(F32) * scale * gpost[layer - 1]
                xbuf[rs, :] = x1

            @pl.when(inside & (k == 0) & (layer < 2))
            def _():
                part = (layer * GROUPS + g) * 2 + s
                x = xbuf[rs, :]
                ybuf[rs, :] = (x * gpre[layer]).astype(BF16)
                sst[part, p] = row_stat(x * x)

                @pl.when(p < top)
                def _():
                    ss_copy(part, p, owner).start()

                @pl.when(p == top)
                def _():
                    for j in range(top):
                        ss_copy(part, j, owner).wait_recv()
                    rss[s] = scale_of(sst, part)

            @pl.when(inside & (layer < 2))
            def _():
                i = layer * n_k + k
                q = layer * per_layer + r
                pbuf[...] = dot(ybuf[rs, :], wgu[i])

                @pl.when(p > 0)
                def _():
                    p_copy(s, q, onward).wait_recv()

                @pl.when(p == 0)
                def _():
                    pslot[s, q] = pbuf[...].astype(BF16)
                    p_copy(s, q, onward).start()

                @pl.when((p > 0) & (p < top))
                def _():
                    pslot[s, q] = (pbuf[...] + pslot[s, q].astype(F32)).astype(BF16)
                    p_copy(s, q, onward).start()

                @pl.when(p == top)
                def _():
                    full = (pbuf[...] + pslot[s, q].astype(F32)) * wide(rss[s], 2 * SLICE)
                    gate = full[:, :SLICE]
                    hslot[s, q] = (gate / (1.0 + jnp.exp(-gate)) * full[:, SLICE:]).astype(BF16)
                    h_copy(s, q, backward).start()

            b = tau - 2 * span + LAG * p
            ok, layer, g, k = item(b)

            @pl.when(ok)
            def _():
                i = layer * n_k + k
                q = (layer * GROUPS + g) * n_k + k
                rs = pl.ds(pl.multiple_of((2 * g + s) * part_rows, part_rows), part_rows)

                @pl.when(p < top)
                def _():
                    h_copy(s, q, backward).wait_recv()

                @pl.when((p < top) & (p > 0))
                def _():
                    h_copy(s, q, backward).start()

                @pl.when(k == 0)
                def _():
                    acc[rs, :] = dot(hslot[s, q], wd[i])

                @pl.when(k > 0)
                def _():
                    acc[rs, :] += dot(hslot[s, q], wd[i])

                @pl.when(k == n_k - 1)
                def _():
                    part = (layer * GROUPS + g) * 2 + s
                    for j in range(2):
                        v1[part, j] = acc[rs, half * j : half * (j + 1)].astype(BF16)
                        a_copy(0, part, j).start()

            ok, layer, g, k = item(b - LAG)

            @pl.when(ok & (k == n_k - 1))
            def _():
                part = (layer * GROUPS + g) * 2 + s
                for j in range(2):
                    a_copy(0, part, j).wait_recv()
                    v2[part, j] = (v1[part, j].astype(F32) + r1[part, j].astype(F32)).astype(BF16)
                    a_copy(1, part, j).start()

            ok, layer, g, k = item(b - 2 * LAG)

            @pl.when(ok & (k == n_k - 1))
            def _():
                part = (layer * GROUPS + g) * 2 + s
                rs = pl.ds(pl.multiple_of((2 * g + s) * part_rows, part_rows), part_rows)
                for j in range(2):
                    a_copy(1, part, j).wait_recv()
                    total = v2[part, j].astype(F32) + r2[part, j].astype(F32)
                    branch[rs, half * j : half * (j + 1)] = total.astype(BF16)
                value = branch[rs, :].astype(F32)
                stats[part, z] = row_stat(value * value)
                for j in range(1, n_ra):
                    st_copy(part, z, j).start()

        return carry

    last = 2 * base + (GROUPS - 1) * n_k + span + 1
    lax.fori_loop(0, last, tick, 0)

    out[...] = xbuf[...]

    def finish(q, carry):
        for s in (0, 1):
            p = z if s == 0 else top - z

            @pl.when(p < top)
            def _():
                p_copy(s, q, z).wait_send()

            @pl.when(p > 0)
            def _():
                h_copy(s, q, z).wait_send()

        return carry

    lax.fori_loop(0, 2 * per_layer, finish, 0)

    def finish_parts(part, carry):
        for phase in range(2):
            for j in range(2):
                a_copy(phase, part, j).wait_send()
        for j in range(1, n_ra):
            st_copy(part, z, j).wait_send()
        s = part % 2
        p = jnp.where(s == 0, z, top - z)

        @pl.when(p < top)
        def _():
            ss_copy(part, p, z).wait_send()

        return carry

    lax.fori_loop(0, 4 * GROUPS, finish_parts, 0)


def shards(n_ra, tokens, g_pre0, gate0, up0, down0, g_post0, g_pre1, gate1, up1, down1, g_post1):
    rows, dl = tokens.shape
    n_k = gate0.shape[1] // SLICE
    parts = 4 * GROUPS
    items = 2 * GROUPS * n_k
    pr = rows // (2 * GROUPS)
    vmem = pl.BlockSpec(memory_space=pltpu.VMEM)
    hbm = pl.BlockSpec(memory_space=pl.ANY)
    dma = pltpu.SemaphoreType.DMA
    row = lambda g: g.reshape(1, dl)
    return pl.pallas_call(
        functools.partial(kernel, n_ra),
        out_shape=jax.ShapeDtypeStruct((rows, dl), F32),
        in_specs=[vmem, vmem, hbm, hbm, hbm, vmem, vmem, hbm, hbm, hbm, vmem],
        out_specs=vmem,
        scratch_shapes=[
            pltpu.VMEM((2 * n_k, dl, 2 * SLICE), BF16),
            pltpu.VMEM((2 * n_k, SLICE, dl), BF16),
            pltpu.VMEM((2, items, pr, 2 * SLICE), BF16),
            pltpu.VMEM((2, items, pr, SLICE), BF16),
            pltpu.VMEM((pr, 2 * SLICE), F32),
            pltpu.VMEM((rows, dl), F32),
            pltpu.VMEM((rows, dl), BF16),
            pltpu.VMEM((rows, dl), F32),
            pltpu.VMEM((rows, dl), BF16),
            pltpu.VMEM((parts, 2, pr, dl // 2), BF16),
            pltpu.VMEM((parts, 2, pr, dl // 2), BF16),
            pltpu.VMEM((parts, 2, pr, dl // 2), BF16),
            pltpu.VMEM((parts, 2, pr, dl // 2), BF16),
            pltpu.VMEM((parts, n_ra, 8, 128), F32),
            pltpu.VMEM((parts, n_ra, 8, 128), F32),
            pltpu.VMEM((2, pr, 128), F32),
            pltpu.VMEM((2, 1, dl), F32),
            pltpu.VMEM((2, 1, dl), F32),
            dma((2 * n_k, 3)),
            dma((2, items)),
            dma((2, items)),
            dma((2, items)),
            dma((2, items)),
            dma((parts, 4)),
            dma((parts, 4)),
            dma((parts, n_ra)),
            dma((parts, n_ra)),
            dma((parts,)),
            dma((parts, n_ra)),
        ],
        compiler_params=pltpu.CompilerParams(
            collective_id=0, has_side_effects=True, vmem_limit_bytes=67043328
        ),
    )(
        tokens, row(g_pre0), gate0, up0, down0, row(g_post0),
        row(g_pre1), gate1, up1, down1, row(g_post1),
    )


def solution(mesh):
    placed = (
        P("dp", "ra"),
        P("ra"),
        P("ra", "cb"),
        P("ra", "cb"),
        P("cb", "ra"),
        P("ra"),
        P("ra"),
        P("ra", "cb"),
        P("ra", "cb"),
        P("cb", "ra"),
        P("ra"),
    )
    return jax.shard_map(
        functools.partial(shards, mesh.shape["ra"]),
        mesh=mesh, in_specs=placed, out_specs=P("dp", "ra"), check_vma=False,
    )
```

```python
import functools

import jax
import jax.numpy as jnp
from jax import lax
from jax.experimental import pallas as pl
from jax.experimental.pallas import tpu as pltpu
from jax.sharding import PartitionSpec as P

EPS = 1e-06
MESH = pl.DeviceIdType.MESH
F32 = jnp.float32
BF16 = jnp.bfloat16
GROUPS = 2
SLICE = 256
LAG = 2
XLAG = 2


def dot(a, b):
    return jnp.dot(a, b, preferred_element_type=F32)


def kernel(
    n_ra, tokens, g_pre0, gate0, up0, down0, g_post0, g_pre1, gate1, up1, down1, g_post1,
    out, wgu, wd, pslot, hslot, gbuf, xbuf, ybuf, acc, branch, v1, r1, v2, r2,
    stats, sst, rss, gpre, gpost,
    w_sem, p_send, p_recv, h_send, h_recv, a_send, a_recv, st_send, st_recv, ss_send, ss_recv,
):
    rows, dl = xbuf.shape
    depth = dl * n_ra
    n_k = gate0.shape[1] // SLICE
    group_rows = rows // GROUPS
    part_rows = group_rows // 2
    per_layer = GROUPS * n_k
    top = n_ra - 1
    span = LAG * top
    ring = gbuf.shape[1]
    base = max(n_k + 2 * span + 3 * XLAG, per_layer)
    half = dl // 2

    z = lax.axis_index("ra")
    c = lax.axis_index("cb")
    x_nb = c + 1 - 2 * (c % 2)
    y_nb = c + 2 - 4 * (c // 2)
    near = jnp.minimum(z, top - z)

    for i in range(2 * n_k):
        layer, k = divmod(i, n_k)
        gate, up, down = ((gate0, up0, down0), (gate1, up1, down1))[layer]
        cols = pl.ds(k * SLICE, SLICE)
        pltpu.make_async_copy(gate.at[:, cols], wgu.at[i, :, pl.ds(0, SLICE)], w_sem.at[i, 0]).start()
        pltpu.make_async_copy(up.at[:, cols], wgu.at[i, :, pl.ds(SLICE, SLICE)], w_sem.at[i, 1]).start()
        pltpu.make_async_copy(down.at[cols, :], wd.at[i], w_sem.at[i, 2]).start()

    barrier = pltpu.get_barrier_semaphore()
    for j in range(1, n_ra):
        pl.semaphore_signal(barrier, inc=1, device_id={"ra": (z + j) % n_ra}, device_id_type=MESH)
    for nb in (x_nb, y_nb):
        pl.semaphore_signal(barrier, inc=1, device_id={"cb": nb}, device_id_type=MESH)

    xbuf[...] = tokens[...].astype(F32)
    gpre[0] = g_pre0[...].astype(F32)
    gpre[1] = g_pre1[...].astype(F32)
    gpost[0] = g_post0[...].astype(F32)
    gpost[1] = g_post1[...].astype(F32)
    pl.semaphore_wait(barrier, n_ra + 1)

    def item(a):
        safe = jnp.maximum(a, 0)
        layer = safe // base
        r = safe % base
        inside = (a >= 0) & (r < per_layer)
        return inside, layer, r // n_k, r % n_k

    def rows_of(g):
        return pl.ds(pl.multiple_of(g * group_rows, group_rows), group_rows)

    def remote(src, dst, send, recv, axis, to):
        return pltpu.make_async_remote_copy(
            src_ref=src, dst_ref=dst, send_sem=send, recv_sem=recv,
            device_id={axis: to}, device_id_type=MESH,
        )

    def p_copy(s, q, to):
        return remote(pslot.at[s, q], pslot.at[s, q], p_send.at[s, q], p_recv.at[s, q], "ra", to)

    def h_copy(s, q, to):
        return remote(hslot.at[q, s], hslot.at[q, s], h_send.at[s, q], h_recv.at[s, q], "ra", to)

    def a_copy(phase, part, j):
        src, dst = ((v1, r1), (v2, r2))[phase]
        to = (x_nb, y_nb)[(phase + j) % 2]
        i = 2 * phase + j
        return remote(src.at[part, j], dst.at[part, j], a_send.at[part, i], a_recv.at[part, i], "cb", to)

    def st_copy(part, src, j):
        to = (z + j) % n_ra
        return remote(stats.at[part, src], stats.at[part, src], st_send.at[part, j], st_recv.at[part, src], "ra", to)

    def ss_copy(part, src, e):
        to = (0, top)[e]
        return remote(sst.at[part, src], sst.at[part, src], ss_send.at[part, e], ss_recv.at[part, src], "ra", to)

    def row_stat(sq):
        lanes = sq[:, 0:128]
        for i in range(1, dl // 128):
            lanes = lanes + sq[:, 128 * i : 128 * (i + 1)]
        got = lax.dot_general(
            jnp.ones((8, 128), F32), lanes, (((1,), (1,)), ((), ())),
            precision=lax.Precision.HIGHEST, preferred_element_type=F32,
        )
        return jnp.concatenate([got] * (128 // group_rows), axis=1)

    def scale_of(ref, part):
        total = ref[part, 0]
        for i in range(1, n_ra):
            total = total + ref[part, i]
        mean = lax.dot_general(
            total[:, 0:group_rows], jnp.full((8, 128), 0.125, F32), (((0,), (0,)), ((), ())),
            precision=lax.Precision.HIGHEST, preferred_element_type=F32,
        )
        return lax.rsqrt(mean / depth + EPS)

    def wide(scale, n):
        return jnp.concatenate([scale] * (n // 128), axis=1)

    def tick(tau, carry):
        inside, layer, g, k = item(tau - LAG * near)

        @pl.when(inside & (k == 0) & (layer >= 1) & (layer <= 2))
        def _():
            part = (layer - 1) * GROUPS + g
            rs = rows_of(g)
            for j in range(1, n_ra):
                st_copy(part, (z + j) % n_ra, j).wait_recv()
            scale = wide(scale_of(stats, part), dl)
            x1 = xbuf[rs, :] + 0.5 * branch[rs, :].astype(F32) * scale * gpost[layer - 1]
            xbuf[rs, :] = x1

        @pl.when(inside & (k == 0) & (layer < 2))
        def _():
            part = layer * GROUPS + g
            rs = rows_of(g)
            x = xbuf[rs, :]
            ybuf[rs, :] = (x * gpre[layer]).astype(BF16)
            sst[part, z] = row_stat(x * x)

            for e in (0, 1):
                @pl.when(z != (0, top)[e])
                def _():
                    ss_copy(part, z, e).start()

        @pl.when(inside & (g == 0) & (layer < 2))
        def _():
            i = layer * n_k + k
            pltpu.make_async_copy(gate0.at[:, pl.ds(0, SLICE)], wgu.at[i, :, pl.ds(0, SLICE)], w_sem.at[i, 0]).wait()
            pltpu.make_async_copy(up0.at[:, pl.ds(0, SLICE)], wgu.at[i, :, pl.ds(SLICE, SLICE)], w_sem.at[i, 1]).wait()

        @pl.when(inside & (layer < 2))
        def _():
            slot = ((layer * GROUPS + g) * n_k + k) % ring
            got = dot(ybuf[rows_of(g), :], wgu[layer * n_k + k])
            gbuf[0, slot] = got[:part_rows]
            gbuf[1, slot] = got[part_rows:]

        for s in (0, 1):
            p = z if s == 0 else top - z
            onward = z + 1 if s == 0 else z - 1
            backward = z - 1 if s == 0 else z + 1

            inside, layer, g, k = item(tau - LAG * p)
            ok = inside & (layer < 2)
            q = (layer * GROUPS + g) * n_k + k

            @pl.when(ok & (p == 0))
            def _():
                pslot[s, q] = gbuf[s, q % ring].astype(BF16)
                p_copy(s, q, onward).start()

            @pl.when(ok & (p > 0) & (p < top))
            def _():
                p_copy(s, q, onward).wait_recv()
                pslot[s, q] = (gbuf[s, q % ring] + pslot[s, q].astype(F32)).astype(BF16)
                p_copy(s, q, onward).start()

            @pl.when(ok & (p == top) & (k == 0))
            def _():
                part = layer * GROUPS + g
                for j in range(1, n_ra):
                    ss_copy(part, (z + j) % n_ra, 0).wait_recv()
                rss[...] = scale_of(sst, part)[part_rows * s : part_rows * (s + 1)]

            @pl.when(ok & (p == top))
            def _():
                p_copy(s, q, onward).wait_recv()
                full = (gbuf[s, q % ring] + pslot[s, q].astype(F32)) * wide(rss[...], 2 * SLICE)
                gate = full[:, :SLICE]
                hslot[q, s] = (gate / (1.0 + jnp.exp(-gate)) * full[:, SLICE:]).astype(BF16)
                h_copy(s, q, backward).start()

            inside, layer, g, k = item(tau - 2 * span + LAG * p)
            ok = inside & (layer < 2)
            q = (layer * GROUPS + g) * n_k + k

            @pl.when(ok & (p < top))
            def _():
                h_copy(s, q, backward).wait_recv()

            @pl.when(ok & (p < top) & (p > 0))
            def _():
                h_copy(s, q, backward).start()

        b = tau - 2 * span + LAG * near
        inside, layer, g, k = item(b)
        ok = inside & (layer < 2)

        @pl.when(ok & (g == 0))
        def _():
            pltpu.make_async_copy(down0.at[pl.ds(0, SLICE), :], wd.at[layer * n_k + k], w_sem.at[layer * n_k + k, 2]).wait()

        @pl.when(ok)
        def _():
            q = (layer * GROUPS + g) * n_k + k
            got = dot(hslot[q].reshape(group_rows, SLICE), wd[layer * n_k + k])

            @pl.when(k == 0)
            def _():
                acc[g] = got

            @pl.when(k > 0)
            def _():
                acc[g] += got

        @pl.when(ok & (k == n_k - 1))
        def _():
            part = layer * GROUPS + g
            for j in range(2):
                v1[part, j] = acc[g, :, half * j : half * (j + 1)].astype(BF16)
                a_copy(0, part, j).start()

        inside, layer, g, k = item(b - XLAG)

        @pl.when(inside & (layer < 2) & (k == n_k - 1))
        def _():
            part = layer * GROUPS + g
            for j in range(2):
                a_copy(0, part, j).wait_recv()
                v2[part, j] = (v1[part, j].astype(F32) + r1[part, j].astype(F32)).astype(BF16)
                a_copy(1, part, j).start()

        inside, layer, g, k = item(b - 2 * XLAG)

        @pl.when(inside & (layer < 2) & (k == n_k - 1))
        def _():
            part = layer * GROUPS + g
            rs = rows_of(g)
            for j in range(2):
                a_copy(1, part, j).wait_recv()
                total = v2[part, j].astype(F32) + r2[part, j].astype(F32)
                branch[rs, half * j : half * (j + 1)] = total.astype(BF16)
            value = branch[rs, :].astype(F32)
            stats[part, z] = row_stat(value * value)
            for j in range(1, n_ra):
                st_copy(part, z, j).start()

        return carry

    last = 2 * base + (GROUPS - 1) * n_k + LAG * (top // 2) + 1
    lax.fori_loop(0, last, tick, 0)

    out[...] = xbuf[...]

    def finish(q, carry):
        for s in (0, 1):
            p = z if s == 0 else top - z

            @pl.when(p < top)
            def _():
                p_copy(s, q, z).wait_send()

            @pl.when(p > 0)
            def _():
                h_copy(s, q, z).wait_send()

        return carry

    lax.fori_loop(0, 2 * per_layer, finish, 0)

    def finish_parts(part, carry):
        for phase in range(2):
            for j in range(2):
                a_copy(phase, part, j).wait_send()
        for j in range(1, n_ra):
            st_copy(part, z, j).wait_send()
        for e in (0, 1):
            @pl.when(z != (0, top)[e])
            def _():
                ss_copy(part, z, e).wait_send()

        return carry

    lax.fori_loop(0, 2 * GROUPS, finish_parts, 0)


def shards(n_ra, tokens, g_pre0, gate0, up0, down0, g_post0, g_pre1, gate1, up1, down1, g_post1):
    rows, dl = tokens.shape
    n_k = gate0.shape[1] // SLICE
    parts = 2 * GROUPS
    items = 2 * GROUPS * n_k
    gr = rows // GROUPS
    pr = gr // 2
    vmem = pl.BlockSpec(memory_space=pltpu.VMEM)
    hbm = pl.BlockSpec(memory_space=pl.ANY)
    dma = pltpu.SemaphoreType.DMA
    row = lambda g: g.reshape(1, dl)
    return pl.pallas_call(
        functools.partial(kernel, n_ra),
        out_shape=jax.ShapeDtypeStruct((rows, dl), F32),
        in_specs=[vmem, vmem, hbm, hbm, hbm, vmem, vmem, hbm, hbm, hbm, vmem],
        out_specs=vmem,
        scratch_shapes=[
            pltpu.VMEM((2 * n_k, dl, 2 * SLICE), BF16),
            pltpu.VMEM((2 * n_k, SLICE, dl), BF16),
            pltpu.VMEM((2, items, pr, 2 * SLICE), BF16),
            pltpu.VMEM((items, 2, pr, SLICE), BF16),
            pltpu.VMEM((2, LAG * (n_ra - 1) + 1, pr, 2 * SLICE), F32),
            pltpu.VMEM((rows, dl), F32),
            pltpu.VMEM((rows, dl), BF16),
            pltpu.VMEM((GROUPS, gr, dl), F32),
            pltpu.VMEM((rows, dl), BF16),
            pltpu.VMEM((parts, 2, gr, dl // 2), BF16),
            pltpu.VMEM((parts, 2, gr, dl // 2), BF16),
            pltpu.VMEM((parts, 2, gr, dl // 2), BF16),
            pltpu.VMEM((parts, 2, gr, dl // 2), BF16),
            pltpu.VMEM((parts, n_ra, 8, 128), F32),
            pltpu.VMEM((parts, n_ra, 8, 128), F32),
            pltpu.VMEM((pr, 128), F32),
            pltpu.VMEM((2, 1, dl), F32),
            pltpu.VMEM((2, 1, dl), F32),
            dma((2 * n_k, 3)),
            dma((2, items)),
            dma((2, items)),
            dma((2, items)),
            dma((2, items)),
            dma((parts, 4)),
            dma((parts, 4)),
            dma((parts, n_ra)),
            dma((parts, n_ra)),
            dma((parts, 2)),
            dma((parts, n_ra)),
        ],
        compiler_params=pltpu.CompilerParams(
            collective_id=0, has_side_effects=True, vmem_limit_bytes=67043328
        ),
    )(
        tokens, row(g_pre0), gate0, up0, down0, row(g_post0),
        row(g_pre1), gate1, up1, down1, row(g_post1),
    )


def solution(mesh):
    placed = (
        P("dp", "ra"),
        P("ra"),
        P("ra", "cb"),
        P("ra", "cb"),
        P("cb", "ra"),
        P("ra"),
        P("ra"),
        P("ra", "cb"),
        P("ra", "cb"),
        P("cb", "ra"),
        P("ra"),
    )
    return jax.shard_map(
        functools.partial(shards, mesh.shape["ra"]),
        mesh=mesh, in_specs=placed, out_specs=P("dp", "ra"), check_vma=False,
    )
```

```python
import functools

import jax
import jax.numpy as jnp
from jax import lax
from jax.experimental import pallas as pl
from jax.experimental.pallas import tpu as pltpu
from jax.sharding import PartitionSpec as P

EPS = 1e-06
MESH = pl.DeviceIdType.MESH
F32 = jnp.float32
BF16 = jnp.bfloat16
GROUPS = 4
SLICE = 256
LAG = 4
XLAG = 5


def dot(a, b):
    return jnp.dot(a, b, preferred_element_type=F32)


def kernel(
    n_ra, tokens, g_pre0, gate0, up0, down0, g_post0, g_pre1, gate1, up1, down1, g_post1,
    out, wgu, wd, pslot, hslot, gbuf, xbuf, ybuf, acc, branch, v1, r1, v2, r2,
    stats, sst, rss, gpre, gpost,
    w_sem, p_send, p_recv, h_send, h_recv, a_send, a_recv, st_send, st_recv, ss_send, ss_recv,
):
    rows, dl = xbuf.shape
    depth = dl * n_ra
    n_k = gate0.shape[1] // SLICE
    group_rows = rows // GROUPS
    part_rows = group_rows // 2
    per_layer = GROUPS * n_k
    top = n_ra - 1
    span = LAG * top
    ring = gbuf.shape[1]
    base = max(n_k + 2 * span + 3 * XLAG, per_layer)
    half = dl // 2

    z = lax.axis_index("ra")
    c = lax.axis_index("cb")
    x_nb = c + 1 - 2 * (c % 2)
    y_nb = c + 2 - 4 * (c // 2)
    near = jnp.minimum(z, top - z)

    for i in range(2 * n_k):
        layer, k = divmod(i, n_k)
        gate, up, down = ((gate0, up0, down0), (gate1, up1, down1))[layer]
        cols = pl.ds(k * SLICE, SLICE)
        pltpu.make_async_copy(gate.at[:, cols], wgu.at[i, :, pl.ds(0, SLICE)], w_sem.at[i, 0]).start()
        pltpu.make_async_copy(up.at[:, cols], wgu.at[i, :, pl.ds(SLICE, SLICE)], w_sem.at[i, 1]).start()
        pltpu.make_async_copy(down.at[cols, :], wd.at[i], w_sem.at[i, 2]).start()

    barrier = pltpu.get_barrier_semaphore()
    for j in range(1, n_ra):
        pl.semaphore_signal(barrier, inc=1, device_id={"ra": (z + j) % n_ra}, device_id_type=MESH)
    for nb in (x_nb, y_nb):
        pl.semaphore_signal(barrier, inc=1, device_id={"cb": nb}, device_id_type=MESH)

    xbuf[...] = tokens[...].astype(F32)
    gpre[0] = g_pre0[...].astype(F32)
    gpre[1] = g_pre1[...].astype(F32)
    gpost[0] = g_post0[...].astype(F32)
    gpost[1] = g_post1[...].astype(F32)
    pl.semaphore_wait(barrier, n_ra + 1)

    def item(a):
        safe = jnp.maximum(a, 0)
        layer = safe // base
        r = safe % base
        inside = (a >= 0) & (r < per_layer)
        return inside, layer, r // n_k, r % n_k

    def rows_of(g):
        return pl.ds(pl.multiple_of(g * group_rows, group_rows), group_rows)

    def remote(src, dst, send, recv, axis, to):
        return pltpu.make_async_remote_copy(
            src_ref=src, dst_ref=dst, send_sem=send, recv_sem=recv,
            device_id={axis: to}, device_id_type=MESH,
        )

    def p_copy(s, q, to):
        return remote(pslot.at[s, q], pslot.at[s, q], p_send.at[s, q], p_recv.at[s, q], "ra", to)

    def h_copy(s, q, to):
        return remote(hslot.at[q, s], hslot.at[q, s], h_send.at[s, q], h_recv.at[s, q], "ra", to)

    def a_copy(phase, part, j):
        src, dst = ((v1, r1), (v2, r2))[phase]
        to = (x_nb, y_nb)[(phase + j) % 2]
        i = 2 * phase + j
        return remote(src.at[part, j], dst.at[part, j], a_send.at[part, i], a_recv.at[part, i], "cb", to)

    def st_copy(part, src, j):
        to = (z + j) % n_ra
        return remote(stats.at[part, src], stats.at[part, src], st_send.at[part, j], st_recv.at[part, src], "ra", to)

    def ss_copy(part, src, e):
        to = (0, top)[e]
        return remote(sst.at[part, src], sst.at[part, src], ss_send.at[part, e], ss_recv.at[part, src], "ra", to)

    def row_stat(sq):
        lanes = sq[:, 0:128]
        for i in range(1, dl // 128):
            lanes = lanes + sq[:, 128 * i : 128 * (i + 1)]
        got = lax.dot_general(
            jnp.ones((8, 128), F32), lanes, (((1,), (1,)), ((), ())),
            precision=lax.Precision.HIGHEST, preferred_element_type=F32,
        )
        return jnp.concatenate([got] * (128 // group_rows), axis=1)

    def scale_of(ref, part):
        total = ref[part, 0]
        for i in range(1, n_ra):
            total = total + ref[part, i]
        mean = lax.dot_general(
            total[:, 0:group_rows], jnp.full((8, 128), 0.125, F32), (((0,), (0,)), ((), ())),
            precision=lax.Precision.HIGHEST, preferred_element_type=F32,
        )
        return lax.rsqrt(mean / depth + EPS)

    def wide(scale, n):
        return jnp.concatenate([scale] * (n // 128), axis=1)

    def tick(tau, carry):
        inside, layer, g, k = item(tau - LAG * near)

        @pl.when(inside & (k == 0) & (layer >= 1) & (layer <= 2))
        def _():
            part = (layer - 1) * GROUPS + g
            rs = rows_of(g)
            for j in range(1, n_ra):
                st_copy(part, (z + j) % n_ra, j).wait_recv()
            scale = wide(scale_of(stats, part), dl)
            x1 = xbuf[rs, :] + 0.5 * branch[rs, :].astype(F32) * scale * gpost[layer - 1]
            xbuf[rs, :] = x1

        @pl.when(inside & (k == 0) & (layer < 2))
        def _():
            part = layer * GROUPS + g
            rs = rows_of(g)
            x = xbuf[rs, :]
            ybuf[rs, :] = (x * gpre[layer]).astype(BF16)
            sst[part, z] = row_stat(x * x)

            for e in (0, 1):
                @pl.when(z != (0, top)[e])
                def _():
                    ss_copy(part, z, e).start()

        @pl.when(inside & (g == 0) & (layer < 2))
        def _():
            i = layer * n_k + k
            pltpu.make_async_copy(gate0.at[:, pl.ds(0, SLICE)], wgu.at[i, :, pl.ds(0, SLICE)], w_sem.at[i, 0]).wait()
            pltpu.make_async_copy(up0.at[:, pl.ds(0, SLICE)], wgu.at[i, :, pl.ds(SLICE, SLICE)], w_sem.at[i, 1]).wait()

        @pl.when(inside & (layer < 2))
        def _():
            slot = ((layer * GROUPS + g) * n_k + k) % ring
            got = dot(ybuf[rows_of(g), :], wgu[layer * n_k + k])
            gbuf[0, slot] = got[:part_rows]
            gbuf[1, slot] = got[part_rows:]

        for s in (0, 1):
            p = z if s == 0 else top - z
            onward = z + 1 if s == 0 else z - 1
            backward = z - 1 if s == 0 else z + 1

            inside, layer, g, k = item(tau - LAG * p)
            ok = inside & (layer < 2)
            q = (layer * GROUPS + g) * n_k + k

            @pl.when(ok & (p == 0))
            def _():
                pslot[s, q] = gbuf[s, q % ring].astype(BF16)
                p_copy(s, q, onward).start()

            @pl.when(ok & (p > 0) & (p < top))
            def _():
                p_copy(s, q, onward).wait_recv()
                pslot[s, q] = (gbuf[s, q % ring] + pslot[s, q].astype(F32)).astype(BF16)
                p_copy(s, q, onward).start()

            @pl.when(ok & (p == top) & (k == 0))
            def _():
                part = layer * GROUPS + g
                for j in range(1, n_ra):
                    ss_copy(part, (z + j) % n_ra, 0).wait_recv()
                rss[...] = scale_of(sst, part)[part_rows * s : part_rows * (s + 1)]

            @pl.when(ok & (p == top))
            def _():
                p_copy(s, q, onward).wait_recv()
                full = (gbuf[s, q % ring] + pslot[s, q].astype(F32)) * wide(rss[...], 2 * SLICE)
                gate = full[:, :SLICE]
                hslot[q, s] = (gate / (1.0 + jnp.exp(-gate)) * full[:, SLICE:]).astype(BF16)
                h_copy(s, q, backward).start()

            inside, layer, g, k = item(tau - 2 * span + LAG * p)
            ok = inside & (layer < 2)
            q = (layer * GROUPS + g) * n_k + k

            @pl.when(ok & (p < top))
            def _():
                h_copy(s, q, backward).wait_recv()

            @pl.when(ok & (p < top) & (p > 0))
            def _():
                h_copy(s, q, backward).start()

        b = tau - 2 * span + LAG * near
        inside, layer, g, k = item(b)
        ok = inside & (layer < 2)

        @pl.when(ok & (g == 0))
        def _():
            pltpu.make_async_copy(down0.at[pl.ds(0, SLICE), :], wd.at[layer * n_k + k], w_sem.at[layer * n_k + k, 2]).wait()

        @pl.when(ok)
        def _():
            q = (layer * GROUPS + g) * n_k + k
            got = dot(hslot[q].reshape(group_rows, SLICE), wd[layer * n_k + k])

            @pl.when(k == 0)
            def _():
                acc[g] = got

            @pl.when(k > 0)
            def _():
                acc[g] += got

        @pl.when(ok & (k == n_k - 1))
        def _():
            part = layer * GROUPS + g
            for j in range(2):
                v1[part, j] = acc[g, :, half * j : half * (j + 1)].astype(BF16)
                a_copy(0, part, j).start()

        inside, layer, g, k = item(b - XLAG)

        @pl.when(inside & (layer < 2) & (k == n_k - 1))
        def _():
            part = layer * GROUPS + g
            for j in range(2):
                a_copy(0, part, j).wait_recv()
                v2[part, j] = (v1[part, j].astype(F32) + r1[part, j].astype(F32)).astype(BF16)
                a_copy(1, part, j).start()

        inside, layer, g, k = item(b - 2 * XLAG)

        @pl.when(inside & (layer < 2) & (k == n_k - 1))
        def _():
            part = layer * GROUPS + g
            rs = rows_of(g)
            for j in range(2):
                a_copy(1, part, j).wait_recv()
                total = v2[part, j].astype(F32) + r2[part, j].astype(F32)
                branch[rs, half * j : half * (j + 1)] = total.astype(BF16)
            value = branch[rs, :].astype(F32)
            stats[part, z] = row_stat(value * value)
            for j in range(1, n_ra):
                st_copy(part, z, j).start()

        return carry

    last = 2 * base + (GROUPS - 1) * n_k + LAG * (top // 2) + 1
    lax.fori_loop(0, last, tick, 0)

    out[...] = xbuf[...]

    def finish(q, carry):
        for s in (0, 1):
            p = z if s == 0 else top - z

            @pl.when(p < top)
            def _():
                p_copy(s, q, z).wait_send()

            @pl.when(p > 0)
            def _():
                h_copy(s, q, z).wait_send()

        return carry

    lax.fori_loop(0, 2 * per_layer, finish, 0)

    def finish_parts(part, carry):
        for phase in range(2):
            for j in range(2):
                a_copy(phase, part, j).wait_send()
        for j in range(1, n_ra):
            st_copy(part, z, j).wait_send()
        for e in (0, 1):
            @pl.when(z != (0, top)[e])
            def _():
                ss_copy(part, z, e).wait_send()

        return carry

    lax.fori_loop(0, 2 * GROUPS, finish_parts, 0)


def shards(n_ra, tokens, g_pre0, gate0, up0, down0, g_post0, g_pre1, gate1, up1, down1, g_post1):
    rows, dl = tokens.shape
    n_k = gate0.shape[1] // SLICE
    parts = 2 * GROUPS
    items = 2 * GROUPS * n_k
    gr = rows // GROUPS
    pr = gr // 2
    vmem = pl.BlockSpec(memory_space=pltpu.VMEM)
    hbm = pl.BlockSpec(memory_space=pl.ANY)
    dma = pltpu.SemaphoreType.DMA
    row = lambda g: g.reshape(1, dl)
    return pl.pallas_call(
        functools.partial(kernel, n_ra),
        out_shape=jax.ShapeDtypeStruct((rows, dl), F32),
        in_specs=[vmem, vmem, hbm, hbm, hbm, vmem, vmem, hbm, hbm, hbm, vmem],
        out_specs=vmem,
        scratch_shapes=[
            pltpu.VMEM((2 * n_k, dl, 2 * SLICE), BF16),
            pltpu.VMEM((2 * n_k, SLICE, dl), BF16),
            pltpu.VMEM((2, items, pr, 2 * SLICE), BF16),
            pltpu.VMEM((items, 2, pr, SLICE), BF16),
            pltpu.VMEM((2, LAG * (n_ra - 1) + 1, pr, 2 * SLICE), F32),
            pltpu.VMEM((rows, dl), F32),
            pltpu.VMEM((rows, dl), BF16),
            pltpu.VMEM((GROUPS, gr, dl), F32),
            pltpu.VMEM((rows, dl), BF16),
            pltpu.VMEM((parts, 2, gr, dl // 2), BF16),
            pltpu.VMEM((parts, 2, gr, dl // 2), BF16),
            pltpu.VMEM((parts, 2, gr, dl // 2), BF16),
            pltpu.VMEM((parts, 2, gr, dl // 2), BF16),
            pltpu.VMEM((parts, n_ra, 8, 128), F32),
            pltpu.VMEM((parts, n_ra, 8, 128), F32),
            pltpu.VMEM((pr, 128), F32),
            pltpu.VMEM((2, 1, dl), F32),
            pltpu.VMEM((2, 1, dl), F32),
            dma((2 * n_k, 3)),
            dma((2, items)),
            dma((2, items)),
            dma((2, items)),
            dma((2, items)),
            dma((parts, 4)),
            dma((parts, 4)),
            dma((parts, n_ra)),
            dma((parts, n_ra)),
            dma((parts, 2)),
            dma((parts, n_ra)),
        ],
        compiler_params=pltpu.CompilerParams(
            collective_id=0, has_side_effects=True, vmem_limit_bytes=67043328
        ),
    )(
        tokens, row(g_pre0), gate0, up0, down0, row(g_post0),
        row(g_pre1), gate1, up1, down1, row(g_post1),
    )


def solution(mesh):
    placed = (
        P("dp", "ra"),
        P("ra"),
        P("ra", "cb"),
        P("ra", "cb"),
        P("cb", "ra"),
        P("ra"),
        P("ra"),
        P("ra", "cb"),
        P("ra", "cb"),
        P("cb", "ra"),
        P("ra"),
    )
    return jax.shard_map(
        functools.partial(shards, mesh.shape["ra"]),
        mesh=mesh, in_specs=placed, out_specs=P("dp", "ra"), check_vma=False,
    )
```
